32 devices in a mesh: sp: 16 (over z, y, core), tp: 2 (over x).
Axes of the slice: x: 2, y: 2, z: 4, core: 2. Of those that a mesh axis runs over, the one named last changes fastest.
Arguments:
- latent: bfloat16 [4096, 2048], P(('sp', 'tp')), may hold values from -36 to 36
- condition: float32 [2048], replicated, may hold values from -16 to 16
- context: bfloat16 [256, 2048], P('sp'), may hold values from -6 to 6
- context_condition_vector: float32 [2048], replicated, may hold values from -6 to 6
- modulation_matrix: bfloat16 [3, 2048, 2048], P(None, 'sp', 'tp'), may hold values from -0.125 to 0.125
- query_matrix: bfloat16 [2048, 2048], P(None, 'tp'), may hold values from -0.125 to 0.125
- key_matrix: bfloat16 [2048, 2048], P(None, 'tp'), may hold values from -0.125 to 0.125
- value_matrix: bfloat16 [2048, 2048], P(None, 'tp'), may hold values from -0.125 to 0.125
- decay_input_weight: bfloat16 [2048, 32], replicated, may hold values from -0.125 to 0.125
- write_strength_weight: bfloat16 [2048, 32], replicated, may hold values from -0.125 to 0.125
- head_decay_rate: float32 [32], replicated, may hold values from 0 to 1, as said below
- write_strength_bias: float32 [32], replicated, may hold values from -20 to 0
- context_write_offset_bias: float32 [32], replicated, may hold values from 1.5 to 4.5
- log_spike_added: float32 [4096, 32], P('sp'), may hold values from -2 to 0, as said below
- head_norm_gain: float32 [128], replicated, may hold values from 0.1 to 1.9
- output_matrix: bfloat16 [2048, 2048], P('tp'), may hold values from -0.125 to 0.125
Outputs:
- mixed: bfloat16 [4096, 2048], P(('sp', 'tp'))
The draws below stay inside these ranges and needn't reach their ends.
Inputs may be any that keep to these rules, and one draw needn't show every extreme that they name: `head_decay_rate`: positive. `log_spike_added`: no entry is positive.
All inputs are finite; a program needn't handle non-finite values.
Results may differ from the reference program's by a relative error of at most 0.018.
Values may be sent and summed in bfloat16 or wider, within the bound.
A program may use at most 128 MiB of HBM per device.

```python
import math
import jax
import jax.numpy as jnp
from jax import lax

D = 2048
RECURRENT_HEADS = 16
DK = 128
BLOCK = 64
TOK_DEV = 256
CTX = 256
LATENT_TOKENS = 4096


def draw_latent(key, part):
    base_key = jax.random.fold_in(key, 11)
    noise_key, row_key, col_key = jax.random.split(base_key, 3)
    noise_part = jnp.clip(jax.random.normal(noise_key, (LATENT_TOKENS, D), jnp.float32), -4.0, 4.0)
    row_scale = jnp.exp(jax.random.uniform(row_key, (LATENT_TOKENS, 1), jnp.float32, math.log(0.3), math.log(3.0)))
    col_scale = jnp.exp(jax.random.uniform(col_key, (1, D), jnp.float32, math.log(0.3), math.log(3.0)))
    return (noise_part * row_scale * col_scale).astype(jnp.bfloat16)


def draw_condition(key, part):
    base_key = jax.random.fold_in(key, 12)
    noise_part = jnp.clip(jax.random.normal(base_key, (D,), jnp.float32), -4.0, 4.0)
    rising = jnp.exp(jnp.linspace(0.0, math.log(3.0), D))
    return noise_part * rising


def draw_head_decay_rate(key, part):
    base_key = jax.random.fold_in(key, 13)
    pick_key, fast_key, slow_key = jax.random.split(base_key, 3)
    fast_heads = jax.random.randint(pick_key, (2 * RECURRENT_HEADS,), 0, 2) == 0
    fast_rate = jnp.exp(jax.random.uniform(fast_key, (2 * RECURRENT_HEADS,), jnp.float32, math.log(0.025), math.log(0.06)))
    slow_rate = jnp.exp(jax.random.uniform(slow_key, (2 * RECURRENT_HEADS,), jnp.float32, math.log(0.05), math.log(0.5))) / LATENT_TOKENS
    return jnp.where(fast_heads, fast_rate, slow_rate)


def draw_write_strength_bias(key, part):
    base_key = jax.random.fold_in(key, 14)
    centre = math.log(DK / (4.0 * LATENT_TOKENS))
    return jax.random.uniform(base_key, (2 * RECURRENT_HEADS,), jnp.float32, centre - 1.0, centre + 1.0)


def draw_log_spike_added(key, part):
    base_key = jax.random.fold_in(key, 15)
    rate_key, location_random_key, magnitude_random_key = jax.random.split(base_key, 3)
    span_length = max(TOK_DEV // 2, 1)
    span_count = LATENT_TOKENS // span_length
    base_rate = jnp.exp(jax.random.uniform(rate_key, (span_count, 2 * RECURRENT_HEADS), jnp.float32, math.log(0.1), math.log(1.0))) / LATENT_TOKENS
    spike_magnitude = jnp.log(jax.random.uniform(magnitude_random_key, (2, 2 * RECURRENT_HEADS), jnp.float32, 0.5, 0.8))
    base_complete = jnp.repeat(base_rate, span_length, axis=0)
    spike_location = jax.random.randint(location_random_key, (2, 2 * RECURRENT_HEADS), 0, LATENT_TOKENS)
    token_position = jnp.arange(LATENT_TOKENS)[:, None, None]
    spike_total = jnp.sum(jnp.where(token_position == spike_location[None], spike_magnitude[None], 0.0), axis=1)
    return spike_total - base_complete


def block_levels(stream_key, dims, shards, low, high):
    def one(dim, shards_of):
        steps = jax.random.uniform(jax.random.fold_in(jax.random.fold_in(stream_key, 6), dim), (shards_of,), jnp.float32, low / len(shards), high / len(shards))
        return jnp.repeat(jnp.exp(steps), dims[dim] // shards_of).reshape((-1,) + (1,) * (len(dims) - dim - 1))

    loudness = one(*shards[0])
    for cut in shards[1:]:
        loudness = loudness * one(*cut)
    return loudness


def scatter_about(rng, shape, scale, limit, cuts=(), kind=jnp.bfloat16):
    gain = block_levels(rng, shape, cuts, -0.22, 0.18) if cuts else 1.0
    entries = jax.random.normal(rng, shape, jnp.float32) * scale * gain
    return jnp.minimum(jnp.maximum(entries, -limit), limit).astype(kind)


def setup_inputs(seed: int = 0) -> dict:
    splits = jax.random.split(jax.random.key(seed), 17)
    latent = draw_latent(jax.random.fold_in(splits[16], 71), 0)
    condition = draw_condition(jax.random.fold_in(splits[16], 71), 0)
    context = scatter_about(splits[2], (CTX, D), 1.0, 6.0, ((0, 16),))
    context_condition_vector = scatter_about(splits[3], (D,), 1.0, 6.0, (), jnp.float32)
    modulation_matrix = scatter_about(splits[4], (3, D, D), D ** -0.5, 0.125, ((1, 16), (2, 2)))
    query_matrix = scatter_about(splits[5], (D, RECURRENT_HEADS * DK), D ** -0.5, 0.125, ((1, 2),))
    key_matrix = scatter_about(splits[6], (D, RECURRENT_HEADS * DK), D ** -0.5, 0.125, ((1, 2),))
    value_matrix = scatter_about(splits[7], (D, RECURRENT_HEADS * DK), D ** -0.5, 0.125, ((1, 2),))
    decay_input_weight = scatter_about(splits[8], (D, 2 * RECURRENT_HEADS), D ** -0.5, 0.125)
    write_strength_weight = scatter_about(splits[9], (D, 2 * RECURRENT_HEADS), D ** -0.5, 0.125)
    head_decay_rate = draw_head_decay_rate(jax.random.fold_in(splits[16], 71), 0)
    write_strength_bias = draw_write_strength_bias(jax.random.fold_in(splits[16], 71), 0)
    context_write_offset_bias = jnp.clip(jax.random.uniform(splits[12], (2 * RECURRENT_HEADS,), jnp.float32, 1.5, 4.5), 1.5, 4.5)
    log_spike_added = draw_log_spike_added(jax.random.fold_in(splits[16], 71), 0)
    head_norm_gain = jnp.clip(1.0 + 0.18 * jax.random.normal(splits[14], (DK,), jnp.float32), 0.1, 1.9)
    output_matrix = scatter_about(splits[15], (RECURRENT_HEADS * DK, D), (RECURRENT_HEADS * DK) ** -0.5, 0.125, ((0, 2),))
    return dict(latent=latent, condition=condition, context=context, context_condition_vector=context_condition_vector, modulation_matrix=modulation_matrix, query_matrix=query_matrix, key_matrix=key_matrix, value_matrix=value_matrix, decay_input_weight=decay_input_weight, write_strength_weight=write_strength_weight, head_decay_rate=head_decay_rate, write_strength_bias=write_strength_bias, context_write_offset_bias=context_write_offset_bias, log_spike_added=log_spike_added, head_norm_gain=head_norm_gain, output_matrix=output_matrix)


EPSILON = 1e-06
TOP_PRECISION = lax.Precision.HIGHEST

def layer_norm(matrix):
    widened = matrix.astype(jnp.float32)
    centred = widened - lax.optimization_barrier(jnp.mean(widened, axis=-1, keepdims=True))
    spread = lax.optimization_barrier(jnp.mean(centred * centred, axis=-1, keepdims=True))
    return centred * lax.rsqrt(spread + EPSILON)

def modulate(matrix, shift_vec, scale_vec):
    return (layer_norm(matrix) * (1.0 + scale_vec) + shift_vec).astype(jnp.bfloat16)

def rounded(matrix):
    return lax.optimization_barrier(matrix.astype(jnp.bfloat16)).astype(jnp.float32)

def project(row_block, weight):
    return rounded(jnp.dot(row_block.astype(jnp.float32), weight.astype(jnp.float32), preferred_element_type=jnp.float32))

def unit_length(vectors):
    return vectors * lax.rsqrt(lax.optimization_barrier(jnp.sum(vectors * vectors, axis=-1, keepdims=True)) + EPSILON)

def orient(matrix, direction):
    return matrix if direction == 0 else jnp.flip(matrix, axis=0)

def to_blocks(matrix):
    block_count = matrix.shape[0] // BLOCK
    shaped = matrix.reshape((block_count, BLOCK) + matrix.shape[1:])
    return jnp.swapaxes(shaped, 1, 2)

def from_blocks(matrix):
    shaped = jnp.swapaxes(matrix, 1, 2)
    return shaped.reshape((shaped.shape[0] * shaped.shape[1],) + shaped.shape[2:])

def block_terms(key_rows, value_rows, logarithm_decay, strength):
    key_blocks = to_blocks(key_rows)
    value_blocks = to_blocks(value_rows)
    strength_blocks = to_blocks(strength)
    cumulative = jnp.cumsum(to_blocks(logarithm_decay), axis=-1)
    token_position = jnp.arange(BLOCK)
    inclusive = token_position[:, None] >= token_position[None, :]
    strictly = token_position[:, None] > token_position[None, :]
    spread_log = cumulative[..., :, None] - cumulative[..., None, :]
    decay_mat = jnp.where(inclusive, jnp.exp(jnp.where(inclusive, spread_log, 0.0)), 0.0)
    weighted = key_blocks * strength_blocks[..., None]
    lower_part = jnp.where(strictly, jnp.einsum('nhid,nhjd->nhij', weighted, key_blocks, precision=TOP_PRECISION) * decay_mat, 0.0)
    system = lower_part + jnp.eye(BLOCK, dtype=jnp.float32)
    right_side = jnp.concatenate([value_blocks * strength_blocks[..., None], weighted * jnp.exp(cumulative)[..., None]], axis=-1)
    solved = jax.scipy.linalg.solve_triangular(system, right_side, lower=True, unit_diagonal=True)
    value_width = value_blocks.shape[-1]
    final_log_value = cumulative[..., -1]
    decayed_keys = key_blocks * jnp.exp(final_log_value[..., None] - cumulative)[..., None]
    return (key_blocks, solved[..., :value_width], solved[..., value_width:], decayed_keys, final_log_value, cumulative, decay_mat)

def advance(carried_state, state_update, correction_term, decayed_keys, final_log_value):
    fresh_values = state_update - jnp.einsum('xui,xij->xuj', correction_term, carried_state, precision=TOP_PRECISION)
    following_rows = carried_state * jnp.exp(final_log_value)[:, None, None] + jnp.einsum('fga,fgo->fao', decayed_keys, fresh_values, precision=TOP_PRECISION)
    return (fresh_values, following_rows)

def final_state(key_rows, value_rows, logarithm_decay, strength, start_state):
    block_parts = block_terms(key_rows, value_rows, logarithm_decay, strength)

    def block_step(carried_state, inputs):
        fresh_values, following_rows = advance(carried_state, *inputs)
        return (following_rows, None)
    carried_state, _ = lax.scan(block_step, start_state, block_parts[1:5])
    return carried_state

def read_out(query_rows, block_parts, start_state):
    key_blocks, state_update, correction_term, decayed_keys, final_log_value, cumulative, decay_mat = block_parts
    query_blocks = to_blocks(query_rows)
    query_decayed = query_blocks * jnp.exp(cumulative)[..., None]
    token_position = jnp.arange(BLOCK)
    inclusive = token_position[:, None] >= token_position[None, :]
    scores = jnp.where(inclusive, jnp.einsum('nhid,nhjd->nhij', query_blocks, key_blocks, precision=TOP_PRECISION) * decay_mat, 0.0)

    def block_step(carried_state, inputs):
        piece_update, piece_fix, piece_keys, piece_log, segment_query, piece_score = inputs
        fresh_values, following_rows = advance(carried_state, piece_update, piece_fix, piece_keys, piece_log)
        result_output = jnp.einsum('xui,xij->xuj', segment_query, carried_state, precision=TOP_PRECISION)
        result_output = result_output + jnp.einsum('hij,hjv->hiv', piece_score, fresh_values, precision=TOP_PRECISION)
        return (following_rows, result_output)
    _, result_output = lax.scan(block_step, start_state, (state_update, correction_term, decayed_keys, final_log_value, query_decayed, scores))
    return from_blocks(result_output)

def reference(latent, condition, context, context_condition_vector, modulation_matrix, query_matrix, key_matrix, value_matrix, decay_input_weight, write_strength_weight, head_decay_rate, write_strength_bias, context_write_offset_bias, log_spike_added, head_norm_gain, output_matrix):
    mod_float = modulation_matrix.astype(jnp.float32)
    latent_factors = jnp.einsum('i,rij->rj', jax.nn.silu(condition), mod_float, precision=TOP_PRECISION)
    context_factors = jnp.einsum('i,rij->rj', jax.nn.silu(context_condition_vector), mod_float[:2], precision=TOP_PRECISION)
    hidden = modulate(latent, latent_factors[0], latent_factors[1])
    context_hidden = modulate(context, context_factors[0], context_factors[1])
    length_total = hidden.shape[0]
    context_length = context_hidden.shape[0]
    queries = project(hidden, query_matrix).reshape(length_total, RECURRENT_HEADS, DK)
    latent_keys = unit_length(project(hidden, key_matrix).reshape(length_total, RECURRENT_HEADS, DK))
    latent_values = project(hidden, value_matrix).reshape(length_total, RECURRENT_HEADS, DK)
    decay_rates = head_decay_rate.reshape(RECURRENT_HEADS, 2)
    logarithm_decay = -decay_rates * jax.nn.softplus(project(hidden, decay_input_weight).reshape(length_total, RECURRENT_HEADS, 2))
    logarithm_decay = logarithm_decay + log_spike_added.reshape(length_total, RECURRENT_HEADS, 2)
    strength = jax.nn.sigmoid(project(hidden, write_strength_weight).reshape(length_total, RECURRENT_HEADS, 2) + write_strength_bias.reshape(RECURRENT_HEADS, 2))
    context_keys = unit_length(project(context_hidden, key_matrix).reshape(context_length, RECURRENT_HEADS, DK))
    context_values = project(context_hidden, value_matrix).reshape(context_length, RECURRENT_HEADS, DK)
    context_decay = -decay_rates * jax.nn.softplus(project(context_hidden, decay_input_weight).reshape(context_length, RECURRENT_HEADS, 2))
    context_strength = jax.nn.sigmoid(project(context_hidden, write_strength_weight).reshape(context_length, RECURRENT_HEADS, 2) + write_strength_bias.reshape(RECURRENT_HEADS, 2) + context_write_offset_bias.reshape(RECURRENT_HEADS, 2))
    zero_state = jnp.zeros((RECURRENT_HEADS, DK, DK), jnp.float32)
    summed = jnp.zeros((length_total, RECURRENT_HEADS, DK), jnp.float32)
    for direction in range(2):
        carried_state = final_state(orient(context_keys, direction), orient(context_values, direction), orient(context_decay[..., direction], direction), orient(context_strength[..., direction], direction), zero_state)
        block_parts = block_terms(orient(latent_keys, direction), orient(latent_values, direction), orient(logarithm_decay[..., direction], direction), orient(strength[..., direction], direction))
        summed = summed + orient(read_out(orient(queries, direction), block_parts, carried_state), direction)
    normed = summed * lax.rsqrt(lax.optimization_barrier(jnp.mean(summed * summed, axis=-1, keepdims=True)) + EPSILON) * head_norm_gain
    normed = normed.astype(jnp.bfloat16).reshape(length_total, RECURRENT_HEADS * DK)
    branch = jnp.dot(normed.astype(jnp.float32), output_matrix.astype(jnp.float32), preferred_element_type=jnp.float32)
    return (latent.astype(jnp.float32) + latent_factors[2] * branch).astype(jnp.bfloat16)
```

```python
import functools

import jax
import jax.numpy as jnp
from jax import lax
from jax.experimental import pallas as pl
from jax.experimental.pallas import tpu as pltpu
from jax.sharding import PartitionSpec as P

DK = 128
HALF = 128
EPSILON = 1e-06
TOP_PRECISION = lax.Precision.HIGHEST
BF = jnp.bfloat16
F32 = jnp.float32


def dot(a, b):
    return jnp.dot(a, b, preferred_element_type=F32)


def layer_norm(matrix):
    widened = matrix.astype(F32)
    centred = widened - jnp.mean(widened, axis=-1, keepdims=True)
    spread = jnp.mean(centred * centred, axis=-1, keepdims=True)
    return centred * lax.rsqrt(spread + EPSILON)


def modulate(matrix, shift_vec, scale_vec):
    return (layer_norm(matrix) * (1.0 + scale_vec) + shift_vec).astype(BF)


def invert_all(lowers):
    size = lowers[0].shape[0]
    rows = lax.broadcasted_iota(jnp.int32, (size, size), 0)
    cols = lax.broadcasted_iota(jnp.int32, (size, size), 1)
    apart = rows ^ cols
    eye = jnp.where(apart == 0, 1.0, 0.0)
    found = [eye - jnp.where(apart == 1, low, 0.0) for low in lowers]
    level = 1
    while (1 << level) < size:
        pick = (apart >> level) == 1
        narrow = [x.astype(BF) for x in found]
        first = [
            dot(x, jnp.where(pick, low, 0.0).astype(BF)).astype(BF)
            for x, low in zip(narrow, lowers)
        ]
        found = [f - dot(t, x) for f, t, x in zip(found, first, narrow)]
        level += 1
    return [x.astype(BF) for x in found]


def unit_rows(raw):
    wide = raw.astype(F32)
    return wide * lax.rsqrt(jnp.sum(wide * wide, axis=-1, keepdims=True) + EPSILON)


def order_masks(length, backward):
    rows = lax.broadcasted_iota(jnp.int32, (length, length), 0)
    cols = lax.broadcasted_iota(jnp.int32, (length, length), 1)
    return (rows < cols, rows <= cols) if backward else (rows > cols, rows >= cols)


def solve_pair(inverses, low, right, backward):
    h = HALF
    if backward:
        last = dot(inverses[1], right[h:].astype(BF)).astype(BF)
        rest = right[:h] - dot(low[:h, h:].astype(BF), last)
        return jnp.concatenate([dot(inverses[0], rest.astype(BF)).astype(BF), last], axis=0)
    head = dot(inverses[0], right[:h].astype(BF)).astype(BF)
    rest = right[h:] - dot(low[h:, :h].astype(BF), head)
    return jnp.concatenate([head, dot(inverses[1], rest.astype(BF)).astype(BF)], axis=0)


def local_kernel(q_ref, k_ref, v_ref, col_ref, row_ref, map_ref, z_ref, y_ref):
    length = q_ref.shape[0]
    h = HALF
    query = q_ref[...]
    keys = unit_rows(k_ref[...])
    values = v_ref[...].astype(F32)
    keys_t = keys.T
    narrow_t = keys_t.astype(BF)
    gram = dot(keys.astype(BF), narrow_t)
    scores = dot(query, narrow_t)
    wide_query = query.astype(F32)
    lows, blocks, reads = [], [], []
    for e in range(2):
        along = col_ref[0, :, e : e + 1]
        across = row_ref[0, e : e + 1, :]
        strength = col_ref[0, :, 2 + e : 3 + e]
        strictly, inclusive = order_masks(length, e == 1)
        decay = jnp.exp(jnp.minimum(along - across, 0.0))
        low = jnp.where(strictly, gram * decay * strength, 0.0)
        lows.append(low)
        reads.append(jnp.where(inclusive, scores * decay, 0.0).astype(BF))
        blocks += [low[:h, :h], low[h:, h:]]
    inverses = invert_all(blocks)
    total = jnp.zeros((length, DK), F32)
    rows = lax.broadcasted_iota(jnp.int32, (DK, DK), 0)
    cols = lax.broadcasted_iota(jnp.int32, (DK, DK), 1)
    for e in range(2):
        along = col_ref[0, :, e : e + 1]
        across = row_ref[0, e : e + 1, :]
        strength = col_ref[0, :, 2 + e : 3 + e]
        grown = jnp.exp(along)
        right = jnp.concatenate([values * strength, keys * (strength * grown)], axis=1)
        solved = solve_pair(inverses[2 * e : 2 * e + 2], lows[e], right, e == 1)
        final = across[:, length - 1 :] if e == 0 else across[:, :1]
        decayed_t = (keys_t * jnp.exp(final - across)).astype(BF)
        both = dot(decayed_t, solved)
        linear = jnp.where(rows == cols, jnp.exp(final), 0.0) - both[:, DK:]
        map_ref[e, 0, 0] = linear.astype(BF)
        map_ref[e, 0, 1] = both[:, :DK].astype(BF)
        seen = dot(reads[e], solved)
        total = total + seen[:, :DK]
        z_ref[0, :, e * DK : (e + 1) * DK] = (wide_query * grown - seen[:, DK:]).astype(BF)
    y_ref[0] = total


def local_terms(q, k, v, col, row, heads, length):
    spec = pl.BlockSpec((length, DK), lambda i: (0, i))
    return pl.pallas_call(
        local_kernel,
        grid=(heads,),
        in_specs=[
            spec,
            spec,
            spec,
            pl.BlockSpec((1, length, 4), lambda i: (i, 0, 0)),
            pl.BlockSpec((1, 2, length), lambda i: (i, 0, 0)),
        ],
        out_specs=[
            pl.BlockSpec((2, 1, 2, DK, DK), lambda i: (0, i, 0, 0, 0)),
            pl.BlockSpec((1, length, 2 * DK), lambda i: (i, 0, 0)),
            pl.BlockSpec((1, length, DK), lambda i: (i, 0, 0)),
        ],
        out_shape=[
            jax.ShapeDtypeStruct((2, heads, 2, DK, DK), BF),
            jax.ShapeDtypeStruct((heads, length, 2 * DK), BF),
            jax.ShapeDtypeStruct((heads, length, DK), F32),
        ],
        cost_estimate=pl.CostEstimate(
            flops=heads * 400 * DK**3, bytes_accessed=heads * 2**20, transcendentals=0
        ),
        name="local_terms",
    )(q, k, v, col, row)


def state_of(raw_keys, raw_values, along, across, strength):
    length = raw_keys.shape[0]
    h = HALF
    keys = unit_rows(raw_keys)
    keys_t = keys.T
    gram = dot(keys.astype(BF), keys_t.astype(BF))
    strictly, _ = order_masks(length, False)
    decay = jnp.exp(jnp.minimum(along - across, 0.0))
    low = jnp.where(strictly, gram * decay * strength, 0.0)
    inverses = invert_all([low[:h, :h], low[h:, h:]])
    solved = solve_pair(inverses, low, raw_values.astype(F32) * strength, False)
    decayed_t = (keys_t * jnp.exp(across[:, length - 1 :] - across)).astype(BF)
    return dot(decayed_t, solved)


def context_kernel(k_ref, v_ref, col_ref, row_ref, out_ref):
    out_ref[0] = state_of(
        k_ref[0], v_ref[0], col_ref[0, :, 0:1], row_ref[0], col_ref[0, :, 1:2]
    )


def context_states(k, v, col, row):
    count, length = k.shape[:2]
    wide = pl.BlockSpec((1, length, DK), lambda i: (i, 0, 0))
    return pl.pallas_call(
        context_kernel,
        grid=(count,),
        in_specs=[
            wide,
            wide,
            pl.BlockSpec((1, length, 2), lambda i: (i, 0, 0)),
            pl.BlockSpec((1, 1, length), lambda i: (i, 0, 0)),
        ],
        out_specs=pl.BlockSpec((1, DK, DK), lambda i: (i, 0, 0)),
        out_shape=jax.ShapeDtypeStruct((count, DK, DK), F32),
        cost_estimate=pl.CostEstimate(
            flops=count * 100 * DK**3, bytes_accessed=count * 2**18, transcendentals=0
        ),
        name="context_states",
    )(k, v, col, row)


def scan_kernel(flag_ref, map_ref, start_ref, out_ref):
    count = map_ref.shape[0]
    back = flag_ref[0]
    state = start_ref[0]
    for lap in range(count):
        source = jnp.where(back == 1, count - 1 - lap, lap)
        narrow = state.astype(BF)
        out_ref[source] = narrow
        if lap < count - 1:
            state = dot(map_ref[source, 0], narrow) + map_ref[source, 1].astype(F32)


def scan_states(flag, maps, start):
    return pl.pallas_call(
        scan_kernel,
        in_specs=[
            pl.BlockSpec(memory_space=pltpu.SMEM),
            pl.BlockSpec(memory_space=pltpu.VMEM),
            pl.BlockSpec(memory_space=pltpu.VMEM),
        ],
        out_specs=pl.BlockSpec(memory_space=pltpu.VMEM),
        out_shape=jax.ShapeDtypeStruct((maps.shape[0], DK, DK), BF),
        name="scan_states",
    )(flag, maps, start)


def read_kernel(z_ref, y_ref, s_ref, gain_ref, out_ref):
    state = s_ref[...].reshape(2 * DK, DK)
    summed = dot(z_ref[0], state) + y_ref[0]
    spread = jnp.mean(summed * summed, axis=-1, keepdims=True)
    out_ref[...] = (summed * lax.rsqrt(spread + EPSILON) * gain_ref[...]).astype(BF)


def read_out(z, y, states, gain):
    heads, length = z.shape[:2]
    return pl.pallas_call(
        read_kernel,
        grid=(heads,),
        in_specs=[
            pl.BlockSpec((1, length, 2 * DK), lambda i: (i, 0, 0)),
            pl.BlockSpec((1, length, DK), lambda i: (i, 0, 0)),
            pl.BlockSpec((2, 1, DK, DK), lambda i: (0, i, 0, 0)),
            pl.BlockSpec((1, DK), lambda i: (0, 0)),
        ],
        out_specs=pl.BlockSpec((length, DK), lambda i: (0, i)),
        out_shape=jax.ShapeDtypeStruct((length, heads * DK), BF),
        name="read_out",
    )(z, y, states, gain)


def gather_rows(matrix, axis):
    if lax.axis_size(axis) != 2:
        return lax.all_gather(matrix, axis, axis=0, tiled=True)
    other = lax.ppermute(matrix, axis, [(0, 1), (1, 0)])
    first = lax.axis_index(axis) == 0
    return jnp.concatenate(
        [jnp.where(first, matrix, other), jnp.where(first, other, matrix)], axis=0
    )


def scatter_sum(normed, weight, axis):
    if lax.axis_size(axis) != 2:
        return lax.psum_scatter(
            dot(normed, weight).astype(BF), axis, scatter_dimension=0, tiled=True
        ).astype(F32)
    rows = normed.shape[0] // 2
    mine = lax.axis_index(axis)
    theirs = dot(lax.dynamic_slice_in_dim(normed, (1 - mine) * rows, rows, 0), weight)
    arrived = lax.ppermute(theirs.astype(BF), axis, [(0, 1), (1, 0)])
    own = dot(lax.dynamic_slice_in_dim(normed, mine * rows, rows, 0), weight)
    return own + arrived.astype(F32)


def running_sums(decay):
    length = decay.shape[0]
    rows = lax.broadcasted_iota(jnp.int32, (length, length), 0)
    cols = lax.broadcasted_iota(jnp.int32, (length, length), 1)
    ahead = jnp.where(rows >= cols, 1.0, 0.0)
    return jnp.dot(ahead, decay, precision=TOP_PRECISION)


def per_device(
    latent,
    condition,
    context,
    context_condition_vector,
    modulation_matrix,
    query_matrix,
    key_matrix,
    value_matrix,
    decay_input_weight,
    write_strength_weight,
    head_decay_rate,
    write_strength_bias,
    context_write_offset_bias,
    log_spike_added,
    head_norm_gain,
    output_matrix,
):
    sp_index = lax.axis_index("sp")
    tp_index = lax.axis_index("tp")
    sp_count = lax.axis_size("sp")
    rows_part = modulation_matrix.shape[1]
    mod_float = modulation_matrix.astype(F32)
    signals = jnp.stack([jax.nn.silu(condition), jax.nn.silu(context_condition_vector)])
    signals = lax.dynamic_slice_in_dim(signals, sp_index * rows_part, rows_part, 1)
    latent_part = jnp.sum(mod_float * signals[0][None, :, None], axis=1)
    context_part = jnp.sum(mod_float[:2] * signals[1][None, :, None], axis=1)
    factors = lax.psum(jnp.concatenate([latent_part, context_part], axis=0), "sp")
    factors = lax.all_gather(factors, "tp", axis=1, tiled=True)

    hidden = gather_rows(modulate(latent, factors[0], factors[1]), "tp")
    context_own = modulate(context, factors[3], factors[4])
    length = hidden.shape[0]
    context_rows = context_own.shape[0]
    heads = query_matrix.shape[1] // DK
    pairs = 2 * heads
    leading = tp_index * pairs

    def columns(matrix):
        return lax.dynamic_slice_in_dim(matrix, leading, pairs, matrix.ndim - 1)

    gate_weight = jnp.concatenate(
        [columns(decay_input_weight), columns(write_strength_weight)], axis=1
    )
    rows_all = jnp.concatenate([hidden, context_own], axis=0)
    queries = dot(hidden, query_matrix).astype(BF)
    keys_raw = dot(rows_all, key_matrix).astype(BF)
    values = dot(rows_all, value_matrix).astype(BF)
    gates = dot(rows_all, gate_weight).astype(BF)

    decay_rates = columns(head_decay_rate)
    write_biases = columns(write_strength_bias)
    context_biases = write_biases + columns(context_write_offset_bias)

    latent_gates = gates[:length].astype(F32)
    log_decay = -decay_rates * jax.nn.softplus(latent_gates[:, :pairs]) + columns(log_spike_added)
    strength = jax.nn.sigmoid(latent_gates[:, pairs:] + write_biases)
    ahead = running_sums(log_decay)
    back = jnp.sum(log_decay, axis=0, keepdims=True) - ahead + log_decay
    forward_column = (jnp.arange(pairs) % 2 == 0)[None, :]
    summed_log = jnp.where(forward_column, ahead, back)
    by_head = summed_log.reshape(length, heads, 2)
    col = jnp.concatenate([by_head, strength.reshape(length, heads, 2)], axis=2).transpose(1, 0, 2)
    row = by_head.transpose(1, 2, 0)
    maps, z, y = local_terms(queries, keys_raw, values, col, row, heads, length)

    context_keys = keys_raw[length:].reshape(context_rows, heads, DK)
    context_values = values[length:].reshape(context_rows, heads, DK)
    context_gates = gates[length:].reshape(context_rows, 2, heads, 2)
    wide = jnp.concatenate([context_keys, context_values], axis=2).transpose(1, 0, 2)
    narrow = context_gates.transpose(3, 2, 0, 1)
    packed = jnp.concatenate(
        [jnp.broadcast_to(wide[None], (2,) + wide.shape), narrow], axis=3
    ).reshape(pairs, context_rows, 2 * DK + 2)
    by_pair = lambda vec: vec.reshape(heads, 2).T.reshape(pairs)
    rates_p, biases_p = by_pair(decay_rates), by_pair(context_biases)

    def context_start(rows, rates, biases, backward):
        rows = jnp.where(backward[:, None, None], rows[:, ::-1], rows)
        raw = rows[:, :, 2 * DK :].astype(F32)
        logs = -rates[:, None] * jax.nn.softplus(raw[:, :, 0])
        power = jax.nn.sigmoid(raw[:, :, 1] + biases[:, None])
        sums = running_sums(logs.T)
        cols = jnp.stack([sums.T, power], axis=2)
        return context_states(
            rows[:, :, :DK], rows[:, :, DK : 2 * DK], cols, sums.T[:, None, :]
        )

    if pairs == sp_count:
        rows = lax.all_to_all(packed, "sp", 0, 0, tiled=True).reshape(1, -1, 2 * DK + 2)
        is_back = (sp_index >= heads).reshape(1)
        take = lambda vec: lax.dynamic_slice_in_dim(vec, sp_index, 1, 0)
        start = context_start(rows, take(rates_p), take(biases_p), is_back)
        arrived = lax.all_to_all(maps.reshape(pairs, 2, DK, DK), "sp", 0, 0, tiled=True)
        prefixes = scan_states(is_back.astype(jnp.int32), arrived, start)
        states = lax.all_to_all(prefixes, "sp", 0, 0, tiled=True).reshape(2, heads, DK, DK)
    else:
        rows = lax.all_gather(packed, "sp", axis=1, tiled=True)
        start = context_start(rows, rates_p, biases_p, jnp.arange(pairs) >= heads)
        start = start.reshape(2, heads, DK, DK)
        gathered = lax.all_gather(maps, "sp")

        def run(e):
            laps = sp_count - 1 - sp_index if e else sp_index

            def one(lap, state):
                source = sp_count - 1 - lap if e else lap
                linear, offset = [
                    lax.dynamic_index_in_dim(gathered[:, e, :, i], source, 0, False)
                    for i in range(2)
                ]
                moved = jnp.einsum(
                    "hij,hjk->hik", linear, state.astype(BF), preferred_element_type=F32
                )
                return moved + offset.astype(F32)

            return lax.fori_loop(0, laps, one, start[e])

        states = jnp.stack([run(0), run(1)]).astype(BF)

    normed = read_out(z, y, states, head_norm_gain[None, :])
    branch = scatter_sum(normed, output_matrix, "tp")
    return (latent.astype(F32) + factors[2] * branch).astype(BF)


def solution(mesh):
    in_specs = (
        P(("sp", "tp"), None),
        P(),
        P("sp", None),
        P(),
        P(None, "sp", "tp"),
        P(None, "tp"),
        P(None, "tp"),
        P(None, "tp"),
        P(),
        P(),
        P(),
        P(),
        P(),
        P("sp", None),
        P(),
        P("tp", None),
    )
    out_specs = P(("sp", "tp"), None)
    return jax.shard_map(
        per_device, mesh=mesh, in_specs=in_specs, out_specs=out_specs, check_vma=False
    )
```

```python
import functools

import jax
import jax.numpy as jnp
from jax import lax
from jax.experimental import pallas as pl
from jax.experimental.pallas import tpu as pltpu
from jax.sharding import PartitionSpec as P

DK = 128
HALF = 128
EPSILON = 1e-06
TOP_PRECISION = lax.Precision.HIGHEST
BF = jnp.bfloat16
F32 = jnp.float32


def dot(a, b):
    return jnp.dot(a, b, preferred_element_type=F32)


def layer_norm(matrix):
    widened = matrix.astype(F32)
    centred = widened - jnp.mean(widened, axis=-1, keepdims=True)
    spread = jnp.mean(centred * centred, axis=-1, keepdims=True)
    return centred * lax.rsqrt(spread + EPSILON)


def modulate(matrix, shift_vec, scale_vec):
    return (layer_norm(matrix) * (1.0 + scale_vec) + shift_vec).astype(BF)


def invert_all(lowers):
    size = lowers[0].shape[0]
    rows = lax.broadcasted_iota(jnp.int32, (size, size), 0)
    cols = lax.broadcasted_iota(jnp.int32, (size, size), 1)
    apart = rows ^ cols
    eye = jnp.where(apart == 0, 1.0, 0.0)
    found = [eye - jnp.where(apart == 1, low, 0.0) for low in lowers]
    level = 1
    while (1 << level) < size:
        pick = (apart >> level) == 1
        narrow = [x.astype(BF) for x in found]
        first = [
            dot(x, jnp.where(pick, low, 0.0).astype(BF)).astype(BF)
            for x, low in zip(narrow, lowers)
        ]
        found = [f - dot(t, x) for f, t, x in zip(found, first, narrow)]
        level += 1
    return [x.astype(BF) for x in found]


def unit_rows(raw):
    wide = raw.astype(F32)
    return wide * lax.rsqrt(jnp.sum(wide * wide, axis=-1, keepdims=True) + EPSILON)


def order_masks(length, backward):
    rows = lax.broadcasted_iota(jnp.int32, (length, length), 0)
    cols = lax.broadcasted_iota(jnp.int32, (length, length), 1)
    return (rows < cols, rows <= cols) if backward else (rows > cols, rows >= cols)


def solve_pair(inverses, low, right, backward):
    h = HALF
    if backward:
        last = dot(inverses[1], right[h:].astype(BF)).astype(BF)
        rest = right[:h] - dot(low[:h, h:].astype(BF), last)
        return jnp.concatenate([dot(inverses[0], rest.astype(BF)).astype(BF), last], axis=0)
    head = dot(inverses[0], right[:h].astype(BF)).astype(BF)
    rest = right[h:] - dot(low[h:, :h].astype(BF), head)
    return jnp.concatenate([head, dot(inverses[1], rest.astype(BF)).astype(BF)], axis=0)


def local_kernel(q_ref, k_ref, v_ref, col_ref, row_ref, map_ref, z_ref, y_ref):
    length = q_ref.shape[0]
    h = HALF
    query = q_ref[...]
    keys = unit_rows(k_ref[...])
    values = v_ref[...].astype(F32)
    keys_t = keys.T
    narrow_t = keys_t.astype(BF)
    gram = dot(keys.astype(BF), narrow_t)
    scores = dot(query, narrow_t)
    wide_query = query.astype(F32)
    lows, blocks, reads = [], [], []
    for e in range(2):
        along = col_ref[0, :, e : e + 1]
        across = row_ref[0, e : e + 1, :]
        strength = col_ref[0, :, 2 + e : 3 + e]
        strictly, inclusive = order_masks(length, e == 1)
        decay = jnp.exp(jnp.minimum(along - across, 0.0))
        low = jnp.where(strictly, gram * decay * strength, 0.0)
        lows.append(low)
        reads.append(jnp.where(inclusive, scores * decay, 0.0).astype(BF))
        blocks += [low[:h, :h], low[h:, h:]]
    inverses = invert_all(blocks)
    total = jnp.zeros((length, DK), F32)
    rows = lax.broadcasted_iota(jnp.int32, (DK, DK), 0)
    cols = lax.broadcasted_iota(jnp.int32, (DK, DK), 1)
    for e in range(2):
        along = col_ref[0, :, e : e + 1]
        across = row_ref[0, e : e + 1, :]
        strength = col_ref[0, :, 2 + e : 3 + e]
        grown = jnp.exp(along)
        right = jnp.concatenate([values * strength, keys * (strength * grown)], axis=1)
        solved = solve_pair(inverses[2 * e : 2 * e + 2], lows[e], right, e == 1)
        final = across[:, length - 1 :] if e == 0 else across[:, :1]
        decayed_t = (keys_t * jnp.exp(final - across)).astype(BF)
        both = dot(decayed_t, solved)
        linear = jnp.where(rows == cols, jnp.exp(final), 0.0) - both[:, DK:]
        map_ref[e, 0, 0] = linear.astype(BF)
        map_ref[e, 0, 1] = both[:, :DK].astype(BF)
        seen = dot(reads[e], solved)
        total = total + seen[:, :DK]
        z_ref[0, :, e * DK : (e + 1) * DK] = (wide_query * grown - seen[:, DK:]).astype(BF)
    y_ref[0] = total


def local_terms(q, k, v, col, row, heads, length):
    spec = pl.BlockSpec((length, DK), lambda i: (0, i))
    return pl.pallas_call(
        local_kernel,
        grid=(heads,),
        in_specs=[
            spec,
            spec,
            spec,
            pl.BlockSpec((1, length, 4), lambda i: (i, 0, 0)),
            pl.BlockSpec((1, 2, length), lambda i: (i, 0, 0)),
        ],
        out_specs=[
            pl.BlockSpec((2, 1, 2, DK, DK), lambda i: (0, i, 0, 0, 0)),
            pl.BlockSpec((1, length, 2 * DK), lambda i: (i, 0, 0)),
            pl.BlockSpec((1, length, DK), lambda i: (i, 0, 0)),
        ],
        out_shape=[
            jax.ShapeDtypeStruct((2, heads, 2, DK, DK), BF),
            jax.ShapeDtypeStruct((heads, length, 2 * DK), BF),
            jax.ShapeDtypeStruct((heads, length, DK), F32),
        ],
        cost_estimate=pl.CostEstimate(
            flops=heads * 400 * DK**3, bytes_accessed=heads * 2**20, transcendentals=0
        ),
        name="local_terms",
    )(q, k, v, col, row)


def state_of(raw_keys, raw_values, along, across, strength):
    length = raw_keys.shape[0]
    h = HALF
    keys = unit_rows(raw_keys)
    keys_t = keys.T
    gram = dot(keys.astype(BF), keys_t.astype(BF))
    strictly, _ = order_masks(length, False)
    decay = jnp.exp(jnp.minimum(along - across, 0.0))
    low = jnp.where(strictly, gram * decay * strength, 0.0)
    inverses = invert_all([low[:h, :h], low[h:, h:]])
    solved = solve_pair(inverses, low, raw_values.astype(F32) * strength, False)
    decayed_t = (keys_t * jnp.exp(across[:, length - 1 :] - across)).astype(BF)
    return dot(decayed_t, solved)


def context_kernel(k_ref, v_ref, col_ref, row_ref, out_ref):
    out_ref[0] = state_of(
        k_ref[0], v_ref[0], col_ref[0, :, 0:1], row_ref[0], col_ref[0, :, 1:2]
    )


def context_states(k, v, col, row):
    count, length = k.shape[:2]
    wide = pl.BlockSpec((1, length, DK), lambda i: (i, 0, 0))
    return pl.pallas_call(
        context_kernel,
        grid=(count,),
        in_specs=[
            wide,
            wide,
            pl.BlockSpec((1, length, 2), lambda i: (i, 0, 0)),
            pl.BlockSpec((1, 1, length), lambda i: (i, 0, 0)),
        ],
        out_specs=pl.BlockSpec((1, DK, DK), lambda i: (i, 0, 0)),
        out_shape=jax.ShapeDtypeStruct((count, DK, DK), F32),
        cost_estimate=pl.CostEstimate(
            flops=count * 100 * DK**3, bytes_accessed=count * 2**18, transcendentals=0
        ),
        name="context_states",
    )(k, v, col, row)


MESH = pl.DeviceIdType.MESH


def greet(peers):
    barrier = pltpu.get_barrier_semaphore()
    for peer in peers:
        pl.semaphore_signal(barrier, inc=1, device_id=peer, device_id_type=MESH)
    pl.semaphore_wait(barrier, len(peers))


def factor_kernel(n, m, x_ref, out_ref, parts, block, sent_a, got_a, sent_b, got_b):
    width = 128
    reducers = x_ref.shape[1] // width
    me, side = lax.axis_index("sp"), lax.axis_index("tp")
    flat = me * m + side
    others = []
    for step in range(1, n * m):
        p = lax.rem(flat + step, n * m)
        others.append((p // m, lax.rem(p, m)))
    greet(others)

    def part(c):
        return pltpu.make_async_remote_copy(
            src_ref=x_ref.at[:, pl.ds(c * width, width)],
            dst_ref=parts.at[me],
            send_sem=sent_a.at[c],
            recv_sem=got_a.at[me],
            device_id=(c, side),
            device_id_type=MESH,
        )

    for c in range(reducers):

        @pl.when(me != c)
        def _():
            part(c).start()

        @pl.when(me == c)
        def _():
            parts[c] = x_ref[:, c * width : (c + 1) * width]

    slot = side * reducers + me

    def whole(step, where):
        return pltpu.make_async_remote_copy(
            src_ref=block,
            dst_ref=out_ref.at[:, pl.ds(pl.multiple_of(where * width, width), width)],
            send_sem=sent_b.at[step],
            recv_sem=got_b.at[where],
            device_id=others[step],
            device_id_type=MESH,
        )

    @pl.when(me < reducers)
    def _():
        for s in range(n):

            @pl.when(me != s)
            def _():
                pltpu.make_async_remote_copy(
                    src_ref=block,
                    dst_ref=parts.at[s],
                    send_sem=sent_a.at[0],
                    recv_sem=got_a.at[s],
                    device_id=others[0],
                    device_id_type=MESH,
                ).wait_recv()

        total = parts[0]
        for s in range(1, n):
            total = total + parts[s]
        block[...] = total
        for step in range(n * m - 1):
            whole(step, slot).start()
        out_ref[:, pl.ds(pl.multiple_of(slot * width, width), width)] = total

    for where in range(m * reducers):

        @pl.when(jnp.logical_or(me != where % reducers, side != where // reducers))
        def _():
            whole(0, where).wait_recv()

    for c in range(reducers):

        @pl.when(me != c)
        def _():
            part(c).wait_send()

    @pl.when(me < reducers)
    def _():
        for step in range(n * m - 1):
            whole(step, slot).wait_send()


def sum_factors(part):
    n, m = lax.axis_size("sp"), lax.axis_size("tp")
    rows, columns = part.shape
    reducers = columns // 128
    return pl.pallas_call(
        functools.partial(factor_kernel, n, m),
        in_specs=[pl.BlockSpec(memory_space=pltpu.VMEM)],
        out_specs=pl.BlockSpec(memory_space=pltpu.VMEM),
        out_shape=jax.ShapeDtypeStruct((rows, m * columns), F32),
        scratch_shapes=[
            pltpu.VMEM((n, rows, 128), F32),
            pltpu.VMEM((rows, 128), F32),
            pltpu.SemaphoreType.DMA((reducers,)),
            pltpu.SemaphoreType.DMA((n,)),
            pltpu.SemaphoreType.DMA((n * m - 1,)),
            pltpu.SemaphoreType.DMA((m * reducers,)),
        ],
        compiler_params=pltpu.CompilerParams(collective_id=1, has_side_effects=True),
        name="sum_factors",
    )(part)


def swap_kernel(n, x_ref, out_ref, sent, got):
    me, side = lax.axis_index("sp"), lax.axis_index("tp")
    peers = [lax.rem(me + step, n) for step in range(1, n)]
    greet([(p, side) for p in peers])
    copies = []
    for step, p in enumerate(peers):
        copy = pltpu.make_async_remote_copy(
            src_ref=x_ref.at[p],
            dst_ref=out_ref.at[me],
            send_sem=sent.at[step],
            recv_sem=got.at[step],
            device_id=(p, side),
            device_id_type=MESH,
        )
        copy.start()
        copies.append(copy)
    out_ref[me] = x_ref[me]
    for copy in copies:
        copy.wait()


def swap_blocks(x):
    n = lax.axis_size("sp")
    return pl.pallas_call(
        functools.partial(swap_kernel, n),
        in_specs=[pl.BlockSpec(memory_space=pltpu.VMEM)],
        out_specs=pl.BlockSpec(memory_space=pltpu.VMEM),
        out_shape=jax.ShapeDtypeStruct(x.shape, x.dtype),
        scratch_shapes=[pltpu.SemaphoreType.DMA((n - 1,)), pltpu.SemaphoreType.DMA((n - 1,))],
        compiler_params=pltpu.CompilerParams(collective_id=2, has_side_effects=True),
        name="swap_blocks",
    )(x)


def exchange_kernel(
    n, map_ref, start_ref, out_ref, held, ready, sent_a, got_a, sent_b, got_b
):
    me, side = lax.axis_index("sp"), lax.axis_index("tp")
    peers = [lax.rem(me + step, n) for step in range(1, n)]
    greet([(p, side) for p in peers])

    def outward(p, source):
        return pltpu.make_async_remote_copy(
            src_ref=map_ref.at[p],
            dst_ref=held.at[source],
            send_sem=sent_a.at[p],
            recv_sem=got_a.at[source],
            device_id=(p, side),
            device_id_type=MESH,
        )

    def homeward(p, source):
        return pltpu.make_async_remote_copy(
            src_ref=ready.at[p],
            dst_ref=out_ref.at[source],
            send_sem=sent_b.at[p],
            recv_sem=got_b.at[source],
            device_id=(p, side),
            device_id_type=MESH,
        )

    for p in peers:
        outward(p, me).start()
    held[me] = map_ref[me]
    back = me // (n // 2)
    state = start_ref[0]
    for lap in range(n):
        source = lap + back * (n - 1 - 2 * lap)
        narrow = state.astype(BF)
        ready[source] = narrow

        @pl.when(source != me)
        def _():
            homeward(source, me).start()
            outward(source, source).wait_recv()

        if lap < n - 1:
            state = dot(held[source, 0], narrow) + held[source, 1].astype(F32)
    out_ref[me] = ready[me]
    for p in peers:
        outward(p, me).wait_send()
        homeward(p, me).wait_send()
        homeward(p, p).wait_recv()


def exchange_states(maps, start):
    n = lax.axis_size("sp")
    return pl.pallas_call(
        functools.partial(exchange_kernel, n),
        in_specs=[pl.BlockSpec(memory_space=pltpu.VMEM)] * 2,
        out_specs=pl.BlockSpec(memory_space=pltpu.VMEM),
        out_shape=jax.ShapeDtypeStruct((n, DK, DK), BF),
        scratch_shapes=[
            pltpu.VMEM(maps.shape, BF),
            pltpu.VMEM((n, DK, DK), BF),
            pltpu.SemaphoreType.DMA((n,)),
            pltpu.SemaphoreType.DMA((n,)),
            pltpu.SemaphoreType.DMA((n,)),
            pltpu.SemaphoreType.DMA((n,)),
        ],
        compiler_params=pltpu.CompilerParams(collective_id=3, has_side_effects=True),
        name="exchange_states",
    )(maps, start)


def read_kernel(z_ref, y_ref, s_ref, gain_ref, out_ref):
    state = s_ref[...].reshape(2 * DK, DK)
    summed = dot(z_ref[0], state) + y_ref[0]
    spread = jnp.mean(summed * summed, axis=-1, keepdims=True)
    out_ref[...] = (summed * lax.rsqrt(spread + EPSILON) * gain_ref[...]).astype(BF)


def read_out(z, y, states, gain):
    heads, length = z.shape[:2]
    return pl.pallas_call(
        read_kernel,
        grid=(heads,),
        in_specs=[
            pl.BlockSpec((1, length, 2 * DK), lambda i: (i, 0, 0)),
            pl.BlockSpec((1, length, DK), lambda i: (i, 0, 0)),
            pl.BlockSpec((2, 1, DK, DK), lambda i: (0, i, 0, 0)),
            pl.BlockSpec((1, DK), lambda i: (0, 0)),
        ],
        out_specs=pl.BlockSpec((length, DK), lambda i: (0, i)),
        out_shape=jax.ShapeDtypeStruct((length, heads * DK), BF),
        name="read_out",
    )(z, y, states, gain)


def gather_rows(matrix, axis):
    if lax.axis_size(axis) != 2:
        return lax.all_gather(matrix, axis, axis=0, tiled=True)
    other = lax.ppermute(matrix, axis, [(0, 1), (1, 0)])
    first = lax.axis_index(axis) == 0
    return jnp.concatenate(
        [jnp.where(first, matrix, other), jnp.where(first, other, matrix)], axis=0
    )


def scatter_sum(normed, weight, axis):
    if lax.axis_size(axis) != 2:
        return lax.psum_scatter(
            dot(normed, weight).astype(BF), axis, scatter_dimension=0, tiled=True
        ).astype(F32)
    rows = normed.shape[0] // 2
    mine = lax.axis_index(axis)
    theirs = dot(lax.dynamic_slice_in_dim(normed, (1 - mine) * rows, rows, 0), weight)
    arrived = lax.ppermute(theirs.astype(BF), axis, [(0, 1), (1, 0)])
    own = dot(lax.dynamic_slice_in_dim(normed, mine * rows, rows, 0), weight)
    return own + arrived.astype(F32)


def running_sums(decay):
    length = decay.shape[0]
    rows = lax.broadcasted_iota(jnp.int32, (length, length), 0)
    cols = lax.broadcasted_iota(jnp.int32, (length, length), 1)
    ahead = jnp.where(rows >= cols, 1.0, 0.0)
    return jnp.dot(ahead, decay, precision=TOP_PRECISION)


def per_device(
    latent,
    condition,
    context,
    context_condition_vector,
    modulation_matrix,
    query_matrix,
    key_matrix,
    value_matrix,
    decay_input_weight,
    write_strength_weight,
    head_decay_rate,
    write_strength_bias,
    context_write_offset_bias,
    log_spike_added,
    head_norm_gain,
    output_matrix,
):
    sp_index = lax.axis_index("sp")
    tp_index = lax.axis_index("tp")
    sp_count = lax.axis_size("sp")
    rows_part = modulation_matrix.shape[1]
    mod_float = modulation_matrix.astype(F32)
    signals = jnp.stack([jax.nn.silu(condition), jax.nn.silu(context_condition_vector)])
    signals = lax.dynamic_slice_in_dim(signals, sp_index * rows_part, rows_part, 1)
    latent_part = jnp.sum(mod_float * signals[0][None, :, None], axis=1)
    context_part = jnp.sum(mod_float[:2] * signals[1][None, :, None], axis=1)
    parts = jnp.concatenate([latent_part, context_part], axis=0)
    whole_pairs = 2 * query_matrix.shape[1] // DK == sp_count
    if whole_pairs and parts.shape[1] // 128 <= sp_count:
        factors = sum_factors(jnp.pad(parts, ((0, 8 - parts.shape[0]), (0, 0))))
    else:
        factors = lax.all_gather(lax.psum(parts, "sp"), "tp", axis=1, tiled=True)

    hidden = gather_rows(modulate(latent, factors[0], factors[1]), "tp")
    context_own = modulate(context, factors[3], factors[4])
    length = hidden.shape[0]
    context_rows = context_own.shape[0]
    heads = query_matrix.shape[1] // DK
    pairs = 2 * heads
    leading = tp_index * pairs

    def columns(matrix):
        return lax.dynamic_slice_in_dim(matrix, leading, pairs, matrix.ndim - 1)

    gate_weight = jnp.concatenate(
        [columns(decay_input_weight), columns(write_strength_weight)], axis=1
    )
    rows_all = jnp.concatenate([hidden, context_own], axis=0)
    queries = dot(hidden, query_matrix).astype(BF)
    keys_raw = dot(rows_all, key_matrix).astype(BF)
    values = dot(rows_all, value_matrix).astype(BF)
    gates = dot(rows_all, gate_weight).astype(BF)

    decay_rates = columns(head_decay_rate)
    write_biases = columns(write_strength_bias)
    context_biases = write_biases + columns(context_write_offset_bias)

    latent_gates = gates[:length].astype(F32)
    log_decay = -decay_rates * jax.nn.softplus(latent_gates[:, :pairs]) + columns(log_spike_added)
    strength = jax.nn.sigmoid(latent_gates[:, pairs:] + write_biases)
    ahead = running_sums(log_decay)
    back = jnp.sum(log_decay, axis=0, keepdims=True) - ahead + log_decay
    forward_column = (jnp.arange(pairs) % 2 == 0)[None, :]
    summed_log = jnp.where(forward_column, ahead, back)
    by_head = summed_log.reshape(length, heads, 2)
    col = jnp.concatenate([by_head, strength.reshape(length, heads, 2)], axis=2).transpose(1, 0, 2)
    row = by_head.transpose(1, 2, 0)
    maps, z, y = local_terms(queries, keys_raw, values, col, row, heads, length)

    context_keys = keys_raw[length:].reshape(context_rows, heads, DK)
    context_values = values[length:].reshape(context_rows, heads, DK)
    context_gates = gates[length:].reshape(context_rows, 2, heads, 2)
    wide = jnp.concatenate([context_keys, context_values], axis=2).transpose(1, 0, 2)
    narrow = context_gates.transpose(3, 2, 0, 1)
    packed = jnp.concatenate(
        [jnp.broadcast_to(wide[None], (2,) + wide.shape), narrow], axis=3
    ).reshape(pairs, context_rows, 2 * DK + 2)
    by_pair = lambda vec: vec.reshape(heads, 2).T.reshape(pairs)
    rates_p, biases_p = by_pair(decay_rates), by_pair(context_biases)

    def context_start(rows, rates, biases, backward):
        rows = jnp.where(backward[:, None, None], rows[:, ::-1], rows)
        raw = rows[:, :, 2 * DK :].astype(F32)
        logs = -rates[:, None] * jax.nn.softplus(raw[:, :, 0])
        power = jax.nn.sigmoid(raw[:, :, 1] + biases[:, None])
        sums = running_sums(logs.T)
        cols = jnp.stack([sums.T, power], axis=2)
        return context_states(
            rows[:, :, :DK], rows[:, :, DK : 2 * DK], cols, sums.T[:, None, :]
        )

    if whole_pairs:
        rows = swap_blocks(packed).reshape(1, -1, 2 * DK + 2)
        is_back = (sp_index >= heads).reshape(1)
        take = lambda vec: lax.dynamic_slice_in_dim(vec, sp_index, 1, 0)
        start = context_start(rows, take(rates_p), take(biases_p), is_back)
        states = exchange_states(maps.reshape(pairs, 2, DK, DK), start)
        states = states.reshape(2, heads, DK, DK)
    else:
        rows = lax.all_gather(packed, "sp", axis=1, tiled=True)
        start = context_start(rows, rates_p, biases_p, jnp.arange(pairs) >= heads)
        start = start.reshape(2, heads, DK, DK)
        gathered = lax.all_gather(maps, "sp")

        def run(e):
            laps = sp_count - 1 - sp_index if e else sp_index

            def one(lap, state):
                source = sp_count - 1 - lap if e else lap
                linear, offset = [
                    lax.dynamic_index_in_dim(gathered[:, e, :, i], source, 0, False)
                    for i in range(2)
                ]
                moved = jnp.einsum(
                    "hij,hjk->hik", linear, state.astype(BF), preferred_element_type=F32
                )
                return moved + offset.astype(F32)

            return lax.fori_loop(0, laps, one, start[e])

        states = jnp.stack([run(0), run(1)]).astype(BF)

    normed = read_out(z, y, states, head_norm_gain[None, :])
    branch = scatter_sum(normed, output_matrix, "tp")
    return (latent.astype(F32) + factors[2] * branch).astype(BF)


def solution(mesh):
    in_specs = (
        P(("sp", "tp"), None),
        P(),
        P("sp", None),
        P(),
        P(None, "sp", "tp"),
        P(None, "tp"),
        P(None, "tp"),
        P(None, "tp"),
        P(),
        P(),
        P(),
        P(),
        P(),
        P("sp", None),
        P(),
        P("tp", None),
    )
    out_specs = P(("sp", "tp"), None)
    return jax.shard_map(
        per_device, mesh=mesh, in_specs=in_specs, out_specs=out_specs, check_vma=False
    )
```
